32 devices in a mesh: sp: 8 (over z, x), tp: 4 (over y, core).
Axes of the slice: x: 2, y: 2, z: 4, core: 2. Of those that a mesh axis runs over, the one named last changes fastest.
Arguments:
- stream: bfloat16 [1024, 2048], P('sp'), may hold values from -15 to 15
- cotangent: bfloat16 [1024, 2048], P('sp'), may hold values from -6 to 6
- route_ids: int32 [1024, 2], P('sp'), may hold values from 0 to 7, all different within a row; in each aligned block of 128 rows (0 to 127, 128 to 255, ...) at most 64 rows name the same one
- route_weights: float32 [1024, 2], P('sp'), may hold values from 0.1 to 0.9
- w_gate: bfloat16 [8, 2048, 2048], P('sp', None, 'tp'), may hold values from -0.125 to 0.125
- w_up: bfloat16 [8, 2048, 2048], P('sp', None, 'tp'), may hold values from -0.125 to 0.125
- w_down: bfloat16 [8, 2048, 2048], P('sp', 'tp'), may hold values from -0.125 to 0.125
- out_proj: bfloat16 [2048, 512], P(None, 'tp'), may hold values from -0.25 to 0.25
- mixed: bfloat16 [512, 1024], P('tp', 'sp'), may hold values from -6 to 6
- rec_input: bfloat16 [512, 1024], P('tp', 'sp'), may hold values from -6 to 6
- branch_input: bfloat16 [512, 1024], P('tp', 'sp'), may hold values from -6 to 6
- state_before: float32 [512, 1024], P('tp', 'sp'), may hold values from -6 to 6
- rec_gates: bfloat16 [16, 32, 32], P('tp'), may hold values from -1 to 1
- in_gates: bfloat16 [16, 32, 32], P('tp'), may hold values from -1 to 1
- decay_param: float32 [512], P('tp'), may hold values from 4.4 to 11
- decay_shift: float32 [512, 1024], P('tp', 'sp'), may hold values from -1.4 to -1e-05
Outputs:
- grad_gate: bfloat16 [8, 2048, 2048], P('sp', None, 'tp')
- grad_up: bfloat16 [8, 2048, 2048], P('sp', None, 'tp')
- grad_down: bfloat16 [8, 2048, 2048], P('sp', 'tp')
- grad_proj: float32 [2048, 512], P('sp', 'tp')
- grad_rec: float32 [512, 1024], P('tp', 'sp')
- grad_branch: float32 [512, 1024], P('tp', 'sp')
The draws below stay inside these ranges and needn't reach their ends.
Inputs may be any that keep to these rules, and one draw needn't show every extreme that they name: `route_ids`: each row names 2 different experts; the rows of one device name no expert more than 64 times, a bound that some block reaches on some device.
All inputs are finite; a program needn't handle non-finite values.
Results may differ from the reference program's by a relative error of at most 0.03.
Values may be sent and summed in bfloat16 or wider, within the bound.
A program may use at most 64 MiB of HBM per device.

```python
import math
import jax
import jax.numpy as jnp
import numpy as np
from jax import lax

D = 2048
F = 2048
W = 512
HD = 32
TOP_K = 2
TOK_DEV = 128
HEADS = 16
EXPERTS = 8
SEQUENCE_TOKENS = 1024
CAP = 64
N_SP = 8
N_TP = 4


def draw_decay_param(key, part):
    pick_key, fast_key, slow_key = jax.random.split(jax.random.fold_in(key, 11), 3)
    slow_share = 0.5
    slow_mask = jax.random.uniform(pick_key, (W,), jnp.float32) < slow_share
    fast_value = jax.random.uniform(fast_key, (W,), jnp.float32, 4.4, 5.2)
    slow_value = jax.random.uniform(slow_key, (W,), jnp.float32, 10.0, 11.0)
    return jnp.where(slow_mask, slow_value, fast_value).astype(jnp.float32)


def draw_decay_shift(key, part):
    block_key, location_key, size_key = jax.random.split(jax.random.fold_in(key, 23), 3)
    block_count = SEQUENCE_TOKENS // TOK_DEV
    block_rate = jax.random.uniform(block_key, (W, block_count), jnp.float32, 2e-05, 0.00015)
    stable_baseline = -jnp.repeat(block_rate, TOK_DEV, axis=1)
    spike_locations = jax.random.randint(location_key, (2,), 0, SEQUENCE_TOKENS)
    retained_fraction = jax.random.uniform(size_key, (2, W), jnp.float32, 0.5, 0.8)
    token_position = jnp.arange(SEQUENCE_TOKENS)
    match_count = token_position[None, None, :] == spike_locations[:, None, None]
    spike_events = jnp.sum(jnp.where(match_count, jnp.log(retained_fraction)[:, :, None], 0.0), axis=0)
    return (stable_baseline + spike_events).astype(jnp.float32)


def raised(entries, rng, source, target, parts, factor):
    def block_of(axis_at):
        return (jnp.arange(entries.shape[axis_at]) // (entries.shape[axis_at] // parts)).reshape((-1,) + (1,) * (entries.ndim - 1 - axis_at))

    first = jax.random.permutation(rng, parts)[block_of(target)]
    second = (block_of(target) + parts // 2) % parts
    return jnp.where((block_of(source) == first) | (block_of(source) == second), factor * entries, entries)


def shard_levels(rng, dims, cuts, low, largest):
    level, own = 1.0, jax.random.fold_in(rng, 6)
    for axis_at, blocks in cuts:
        heights = jnp.exp(jax.random.uniform(jax.random.fold_in(own, axis_at), (blocks,), jnp.float32, low / len(cuts), largest / len(cuts)))
        level = level * jnp.repeat(heights, dims[axis_at] // blocks).reshape([-1 if axis == axis_at else 1 for axis in range(len(dims))])
    return level


def shared_out(stream_key, own, number, rows, amount, top, limit, skew):
    order = jax.random.permutation(stream_key, amount)
    packed, ordinary = load_shares(amount, rows * top, limit, skew, True), load_shares(amount, rows * top, limit, skew, False)
    places = jnp.arange(amount)

    def named(tallies, turn):
        used = int((tallies > 0).sum())
        fixed = max(1, used // 4)
        passed = fixed + (places - fixed + turn * (used - fixed)) % max(1, amount - fixed)
        return jnp.zeros((amount,), jnp.int32).at[order[jnp.where(places < fixed, places, passed)]].set(jnp.asarray(tallies, jnp.int32))

    tallies = jnp.where(number % 4 == 0, named(packed, number // 4), named(ordinary, number - number // 4 - 1))
    mixed = jax.random.permutation(jax.random.fold_in(own, 3), amount)
    source_of, sink = mixed[0:amount // 2 * 2:2], mixed[1:amount // 2 * 2:2]
    room = jnp.minimum(tallies[source_of] - 1, limit - tallies[sink]) // 2
    room = jnp.where((source_of == order[0]) | (sink == order[0]) | (tallies[sink] == 0), 0, jnp.maximum(room, 0))
    passed = jax.random.randint(jax.random.fold_in(own, 4), (amount // 2,), 0, 1 << 20) % (room + 1)
    tallies = tallies.at[source_of].add(-passed).at[sink].add(passed)
    members = jnp.searchsorted(jnp.cumsum(tallies), jnp.arange(rows * top), side="right").astype(jnp.int32)
    grid = members.reshape(top, rows).T
    grid = grid[jax.random.permutation(jax.random.fold_in(own, 1), rows)]
    turn = jax.random.randint(jax.random.fold_in(own, 2), (rows, 1), 0, top)
    return jnp.take_along_axis(grid, (jnp.arange(top)[None, :] + turn) % top, axis=1)


def load_shares(amount, total, most, lean, full):
    portions = [(1 << 20) // math.isqrt(rank ** lean) + 1 for rank in range(1, amount + 1)]
    largest = most if full else min(most, max(-(-total // amount), total * portions[0] // sum(portions)))
    least = 1 if total - largest >= amount - 1 else 0
    counts, spare = [largest] + [least] * (amount - 1), total - largest - least * (amount - 1)
    while spare > 0:
        candidates = [i for i in range(1, amount) if counts[i] < largest] or [i for i in range(1, amount) if counts[i] < most]
        mass, budget = sum([portions[i] for i in candidates]), spare
        for i in candidates:
            addition = min(most - counts[i], max(1, budget * portions[i] // mass), spare)
            counts[i] = counts[i] + addition
            spare = spare - addition
    return np.array(counts)


def noise(key, extent, spread, bound, cuts=(), held_as=jnp.bfloat16):
    factor_of = shard_levels(key, extent, cuts, -0.22, 0.18) if cuts else 1.0
    drawn = jax.random.normal(key, extent, jnp.float32) * spread * factor_of
    return jnp.minimum(jnp.maximum(drawn, -bound), bound).astype(held_as)


def noise_with(own_key, shape, width, most, cuts, heavy, kind=jnp.bfloat16):
    array = width * jax.random.normal(own_key, shape, jnp.float32)
    if cuts:
        array = array * shard_levels(own_key, shape, cuts, -0.22, 0.18)
    return jnp.clip(raised(array, jax.random.fold_in(own_key, 3), *heavy), -most, most).astype(kind)


def setup_inputs(seed: int = 0) -> dict:
    arg_keys = jax.random.split(jax.random.key(seed), 17)
    stream = noise(arg_keys[0], (SEQUENCE_TOKENS, D), 2.5, 15.0, ((0, 8),))
    cotangent = noise_with(arg_keys[1], (SEQUENCE_TOKENS, D), 1.0, 6.0, ((0, 8),), (0, 1, 8, 2.0))
    route_ids_keys = jax.random.split(jax.random.fold_in(arg_keys[2], 1), SEQUENCE_TOKENS // TOK_DEV)
    route_ids_turns = jax.random.permutation(jax.random.fold_in(arg_keys[2], 3), SEQUENCE_TOKENS // TOK_DEV)
    route_ids = jax.vmap(lambda own, number: shared_out(jax.random.fold_in(arg_keys[2], 2), own, number, TOK_DEV, EXPERTS, TOP_K, CAP, 1))(route_ids_keys, route_ids_turns).reshape((SEQUENCE_TOKENS, TOP_K))
    route_weights = jnp.clip(0.1 + 0.79999997 * jax.random.uniform(arg_keys[3], (SEQUENCE_TOKENS, TOP_K), jnp.float32) ** shard_levels(arg_keys[3], (SEQUENCE_TOKENS, TOP_K), ((0, 8),), -0.2, 0.2), 0.1, 0.9)
    w_gate = noise(arg_keys[4], (EXPERTS, D, F), D ** -0.5, 0.125, ((0, 8), (2, 4)))
    w_up = noise(arg_keys[5], (EXPERTS, D, F), D ** -0.5, 0.125, ((0, 8), (2, 4)))
    w_down = noise(arg_keys[6], (EXPERTS, F, D), F ** -0.5, 0.125, ((0, 8), (1, 4)))
    out_proj = noise(arg_keys[7], (D, W), W ** -0.5, 0.25, ((1, 4),))
    mixed = noise(arg_keys[8], (W, SEQUENCE_TOKENS), 1.0, 6.0, ((0, 4), (1, 8)))
    rec_input = noise(arg_keys[9], (W, SEQUENCE_TOKENS), 1.0, 6.0, ((0, 4), (1, 8)))
    branch_input = noise(arg_keys[10], (W, SEQUENCE_TOKENS), 1.0, 6.0, ((0, 4), (1, 8)))
    state_before = noise(arg_keys[11], (W, SEQUENCE_TOKENS), 1.0, 6.0, ((0, 4), (1, 8)), jnp.float32)
    rec_gates = noise(arg_keys[12], (HEADS, HD, HD), HD ** -0.5, 1.0, ((0, 4),))
    in_gates = noise(arg_keys[13], (HEADS, HD, HD), HD ** -0.5, 1.0, ((0, 4),))
    decay_param = draw_decay_param(jax.random.fold_in(arg_keys[16], 71), 0)
    decay_shift = draw_decay_shift(jax.random.fold_in(arg_keys[16], 71), 0)
    return {"stream": stream, "cotangent": cotangent, "route_ids": route_ids, "route_weights": route_weights, "w_gate": w_gate, "w_up": w_up, "w_down": w_down, "out_proj": out_proj, "mixed": mixed, "rec_input": rec_input, "branch_input": branch_input, "state_before": state_before, "rec_gates": rec_gates, "in_gates": in_gates, "decay_param": decay_param, "decay_shift": decay_shift}


RATE_SCALE = 8.0
CLAMP_LIMIT = 7.0
GLU_ALPHA = 1.702

def expert_act(gate_pre, up_pre):
    glu_part = jnp.minimum(gate_pre, CLAMP_LIMIT)
    lin_part = jnp.clip(up_pre, -CLAMP_LIMIT, CLAMP_LIMIT)
    return glu_part * jax.nn.sigmoid(GLU_ALPHA * glu_part) * (lin_part + 1.0)

def reverse_step(later_elem, earlier_elem):
    return (later_elem[0] * earlier_elem[0], earlier_elem[1] + earlier_elem[0] * later_elem[1])

def reference(stream, cotangent, route_ids, route_weights, w_gate, w_up, w_down, out_proj, mixed, rec_input, branch_input, state_before, rec_gates, in_gates, decay_param, decay_shift):
    token_count, model_width = cotangent.shape
    top_count = route_ids.shape[1]
    expert_count = w_gate.shape[0]
    hidden = w_gate.shape[2]
    per_device = token_count // N_SP
    capacity = 2 * per_device * top_count // expert_count
    expert_rows = N_SP * capacity
    grouped = route_ids.reshape(N_SP, per_device * top_count)
    onehot = (grouped[:, :, None] == jnp.arange(expert_count, dtype=jnp.int32)[None, None, :]).astype(jnp.int32)
    slot_index = lax.optimization_barrier(jnp.sum((jnp.cumsum(onehot, axis=1) - onehot) * onehot, axis=2))
    device_ids = jnp.arange(N_SP, dtype=jnp.int32)[:, None]
    target = (grouped * expert_rows + device_ids * capacity + slot_index).reshape(-1).astype(jnp.int32)
    scaled = (route_weights[:, :, None] * cotangent[:, None, :].astype(jnp.float32)).astype(jnp.bfloat16)
    scaled = scaled.reshape(-1, model_width)
    copies = jnp.broadcast_to(stream[:, None, :], (token_count, top_count, model_width)).reshape(-1, model_width)
    empty_rows = jnp.zeros((expert_count * expert_rows, model_width), jnp.bfloat16)
    grad_rows = empty_rows.at[target].set(scaled).reshape(expert_count, expert_rows, model_width)
    token_rows = empty_rows.at[target].set(copies).reshape(expert_count, expert_rows, model_width)
    group_width = hidden // N_TP

    def one_expert(expert_item):
        grads_one, tokens_one, gate_one, up_one, down_one = expert_item
        gate_pre = jnp.dot(tokens_one, gate_one, preferred_element_type=jnp.float32)
        up_pre = jnp.dot(tokens_one, up_one, preferred_element_type=jnp.float32)
        act_val, act_vjp = jax.vjp(expert_act, gate_pre, up_pre)
        act_low = act_val.astype(jnp.bfloat16)
        d_act = jnp.dot(grads_one, down_one.T, preferred_element_type=jnp.float32)
        d_gate, d_up = act_vjp(d_act)
        d_gate = d_gate.astype(jnp.bfloat16)
        d_up = d_up.astype(jnp.bfloat16)
        g_gate = jnp.dot(tokens_one.T, d_gate, preferred_element_type=jnp.float32).astype(jnp.bfloat16)
        g_up = jnp.dot(tokens_one.T, d_up, preferred_element_type=jnp.float32).astype(jnp.bfloat16)
        g_down = jnp.dot(act_low.T, grads_one, preferred_element_type=jnp.float32).astype(jnp.bfloat16)
        gate_terms = jnp.einsum('rjf,djf->jrd', d_gate.astype(jnp.float32).reshape(expert_rows, N_TP, group_width), gate_one.astype(jnp.float32).reshape(model_width, N_TP, group_width))
        up_terms = jnp.einsum('rjf,djf->jrd', d_up.astype(jnp.float32).reshape(expert_rows, N_TP, group_width), up_one.astype(jnp.float32).reshape(model_width, N_TP, group_width))
        rounded = lax.optimization_barrier((gate_terms + up_terms).astype(jnp.bfloat16))
        summed = lax.optimization_barrier(jnp.sum(rounded.astype(jnp.float32), axis=0)).astype(jnp.bfloat16)
        return (g_gate, g_up, g_down, summed)
    grad_gate, grad_up, grad_down, slot_grads = lax.map(one_expert, (grad_rows, token_rows, w_gate, w_up, w_down))
    per_pair = slot_grads.reshape(-1, model_width)[target].astype(jnp.float32).reshape(token_count, top_count, model_width)
    stream_low = (cotangent.astype(jnp.float32) + lax.optimization_barrier(jnp.sum(per_pair, axis=1))).astype(jnp.bfloat16)
    d_mixed = lax.dot_general(out_proj, stream_low, (((0,), (1,)), ((), ())), preferred_element_type=jnp.float32)
    grad_proj = lax.dot_general(stream_low, mixed, (((0,), (1,)), ((), ())), preferred_element_type=jnp.float32)
    channels, positions = rec_input.shape
    gate_heads = rec_gates.shape[0]
    head_dim = rec_gates.shape[1]
    rec_value = rec_input.astype(jnp.float32)
    rec_heads = rec_value.reshape(gate_heads, head_dim, positions)
    rec_pre = jnp.einsum('hij,hit->hjt', rec_gates.astype(jnp.float32), rec_heads).reshape(channels, positions)
    in_pre = jnp.einsum('hij,hit->hjt', in_gates.astype(jnp.float32), rec_heads).reshape(channels, positions)
    rec_gate = jax.nn.sigmoid(rec_pre)
    in_gate = jax.nn.sigmoid(in_pre)
    soft_plus = jax.nn.softplus(-decay_param)[:, None]
    log_decay = -RATE_SCALE * rec_gate * soft_plus + decay_shift
    decay_rate = jnp.exp(log_decay)
    at_start = (jnp.arange(positions) == 0)[None, :]
    raw_mult = jnp.sqrt(-jnp.expm1(2.0 * log_decay))
    multiplier = jnp.where(at_start, 1.0, raw_mult)
    state_now = decay_rate * state_before + multiplier * in_gate * rec_value
    gelu_val, gelu_vjp = jax.vjp(jax.nn.gelu, branch_input.astype(jnp.float32))
    grad_branch = gelu_vjp(d_mixed * state_now)[0]
    d_state = d_mixed * gelu_val
    next_decay = jnp.concatenate([decay_rate[:, 1:], jnp.zeros((channels, 1), jnp.float32)], axis=1)
    adjoint = lax.associative_scan(reverse_step, (next_decay, d_state), reverse=True, axis=1)[1]
    mult_term = adjoint * in_gate * rec_value * decay_rate * decay_rate / raw_mult
    d_log = adjoint * state_before * decay_rate - jnp.where(at_start, 0.0, mult_term)
    d_rec_pre = (d_log * -RATE_SCALE * soft_plus * rec_gate * (1.0 - rec_gate)).astype(jnp.bfloat16)
    d_in_pre = (adjoint * multiplier * rec_value * in_gate * (1.0 - in_gate)).astype(jnp.bfloat16)
    d_rec_pre, d_in_pre = lax.optimization_barrier((d_rec_pre, d_in_pre))
    back_rec = jnp.einsum('hij,hjt->hit', rec_gates.astype(jnp.float32), d_rec_pre.astype(jnp.float32).reshape(gate_heads, head_dim, positions))
    back_in = jnp.einsum('hij,hjt->hit', in_gates.astype(jnp.float32), d_in_pre.astype(jnp.float32).reshape(gate_heads, head_dim, positions))
    grad_rec = adjoint * multiplier * in_gate + (back_rec + back_in).reshape(channels, positions)
    return (grad_gate, grad_up, grad_down, grad_proj, grad_rec, grad_branch)
```

```python
import functools

import jax
import jax.numpy as jnp
from jax import lax
from jax.experimental import pallas as pl
from jax.experimental.pallas import tpu as pltpu
from jax.sharding import PartitionSpec as P

RATE_SCALE = 8.0
CLAMP_LIMIT = 7.0
GLU_ALPHA = 1.702
CORES = 2
MESH = pl.DeviceIdType.MESH
VMEM_LIMIT = 60 * 1024 * 1024


def expert_act(gate_pre, up_pre):
    glu_part = jnp.minimum(gate_pre, CLAMP_LIMIT)
    lin_part = jnp.clip(up_pre, -CLAMP_LIMIT, CLAMP_LIMIT)
    return glu_part * jax.nn.sigmoid(GLU_ALPHA * glu_part) * (lin_part + 1.0)


def reverse_step(later_elem, earlier_elem):
    return (later_elem[0] * earlier_elem[0], earlier_elem[1] + earlier_elem[0] * later_elem[1])


def weight_grads(tokens_in, grads_in, d_gate, d_up, act_low):
    g_gate = jnp.einsum("secd,secf->edf", tokens_in, d_gate, preferred_element_type=jnp.float32)
    g_up = jnp.einsum("secd,secf->edf", tokens_in, d_up, preferred_element_type=jnp.float32)
    g_down = jnp.einsum("secf,secd->efd", act_low, grads_in, preferred_element_type=jnp.float32)
    return (g_gate.astype(jnp.bfloat16), g_up.astype(jnp.bfloat16), g_down.astype(jnp.bfloat16))


def aligned(value, size):
    return pl.multiple_of(value * size, size)


def remote(src, dst, send_sem, recv_sem, device):
    return pltpu.make_async_remote_copy(
        src_ref=src,
        dst_ref=dst,
        send_sem=send_sem,
        recv_sem=recv_sem,
        device_id=device,
        device_id_type=MESH,
    )


class Place:
    def __init__(self, n_sp, n_tp):
        self.n, self.ny = n_sp, n_tp // CORES
        self.s, self.t = lax.axis_index("sp"), lax.axis_index("tp")
        self.y, self.c = self.t // CORES, lax.rem(self.t, CORES)
        self.partner = (self.s, self.y * CORES + 1 - self.c)

    def sp_peer(self, i):
        return lax.rem(self.s + i, self.n)

    def sp_source(self, i):
        return lax.rem(self.s + self.n - i, self.n)

    def y_peer(self, j):
        return lax.rem(self.y + j, self.ny)

    def y_source(self, j):
        return lax.rem(self.y + self.ny - j, self.ny)

    def tp_of(self, y, c):
        return y * CORES + c

    def barrier(self, along_tp=True):
        sem = pltpu.get_barrier_semaphore()

        def greet(device):
            pl.semaphore_signal(sem, inc=1, device_id=device, device_id_type=MESH)

        for i in range(1, self.n):
            greet((self.sp_peer(i), self.t))
        count = self.n - 1
        if along_tp:
            for j in range(1, self.ny):
                greet((self.s, self.tp_of(self.y_peer(j), self.c)))
            greet(self.partner)
            count += self.ny
        pl.semaphore_wait(sem, count)


def dispatch_kernel(
    n_sp, n_tp, tok_src, grd_src, tok_out, grd_out, own_sem, sa, ra, sy, ry, sc, rc
):
    at = Place(n_sp, n_tp)
    rows = tok_src.shape[0] // n_sp
    cols = tok_src.shape[1]
    pairs = ((tok_src, tok_out), (grd_src, grd_out))

    def block(out, source, tp):
        return out.at[pl.ds(aligned(source, rows), rows), pl.ds(aligned(tp, cols), cols)]

    def first(a, i):
        src, out = pairs[a]
        peer = at.sp_peer(i)
        return remote(
            src.at[pl.ds(aligned(peer, rows), rows), :],
            block(out, at.s, at.t),
            sa.at[a, i],
            ra.at[a, i],
            (peer, at.t),
        )

    def along_y(a, i, j, source, outgoing):
        src, out = pairs[a]
        tp = at.t if outgoing else at.tp_of(at.y_source(j), at.c)
        spot = block(out, source, tp)
        return remote(
            spot, spot, sy.at[a, i, j], ry.at[a, i, j], (at.s, at.tp_of(at.y_peer(j), at.c))
        )

    def across(a, i, j, source, outgoing):
        src, out = pairs[a]
        tp = at.tp_of(at.y_source(j), at.c if outgoing else 1 - at.c)
        spot = block(out, source, tp)
        return remote(spot, spot, sc.at[a, i, j], rc.at[a, i, j], at.partner)

    own = []
    for a in range(2):
        src, out = pairs[a]
        copy = pltpu.make_async_copy(
            src.at[pl.ds(aligned(at.s, rows), rows), :], block(out, at.s, at.t), own_sem.at[a]
        )
        copy.start()
        own.append(copy)
    at.barrier()

    for a in range(2):

        def send(i, _):
            first(a, i).start()
            return 0

        lax.fori_loop(1, n_sp, send, 0)
    for copy in own:
        copy.wait()

    def pass_on(a, i):
        source = at.sp_source(i)
        for j in range(1, at.ny):
            along_y(a, i, j, source, True).start()
        across(a, i, 0, source, True).start()

    def relay(a, i):
        source = at.sp_source(i)
        for j in range(1, at.ny):
            along_y(a, i, j, source, False).wait_recv()
            across(a, i, j, source, True).start()

    for a in range(2):
        pass_on(a, 0)
    for a in range(2):

        def step(i, _):
            first(a, i).wait_recv()
            pass_on(a, i)
            relay(a, i - 1)
            return 0

        lax.fori_loop(1, n_sp, step, 0)
        relay(a, n_sp - 1)

    for a in range(2):

        def drain(i, _):
            source = at.sp_source(i)
            for j in range(at.ny):
                across(a, i, j, source, False).wait_recv()
                across(a, i, j, source, True).wait_send()
            for j in range(1, at.ny):
                along_y(a, i, j, source, True).wait_send()
            return 0

        def drain_first(i, _):
            first(a, i).wait_send()
            return 0

        lax.fori_loop(0, n_sp, drain, 0)
        lax.fori_loop(1, n_sp, drain_first, 0)


def dispatch(tok_src, grd_src, n_sp, n_tp):
    total, cols = tok_src.shape
    ny = n_tp // CORES
    dma = pltpu.SemaphoreType.DMA
    shape = jax.ShapeDtypeStruct((total, cols * n_tp), jnp.bfloat16)
    return pl.pallas_call(
        functools.partial(dispatch_kernel, n_sp, n_tp),
        out_shape=(shape, shape),
        in_specs=[pl.BlockSpec(memory_space=pltpu.VMEM)] * 2,
        out_specs=[pl.BlockSpec(memory_space=pl.ANY)] * 2,
        scratch_shapes=[
            dma((2,)),
            dma((2, n_sp)),
            dma((2, n_sp)),
            dma((2, n_sp, ny)),
            dma((2, n_sp, ny)),
            dma((2, n_sp, ny)),
            dma((2, n_sp, ny)),
        ],
        compiler_params=pltpu.CompilerParams(
            collective_id=0, has_side_effects=True, vmem_limit_bytes=VMEM_LIMIT
        ),
    )(tok_src, grd_src)


def return_kernel(
    n_sp, n_tp, part, pick, cot, out,
    core_in, own_sum, y_out, y_in, ret_out, ret_in, low,
    sc, rc, sy, ry, sr, rr, sl, rl, sp_, rp_, own_sem,
):
    at = Place(n_sp, n_tp)
    rows = part.shape[0] // n_sp
    cols = part.shape[1] // n_tp
    tok = cot.shape[0]

    def piece(peer, tp):
        return pl.ds(aligned(peer, rows), rows), pl.ds(aligned(tp, cols), cols)

    def peer_of(i):
        return at.sp_peer(i + 1)

    def core_copy(i, j):
        r, c = piece(peer_of(i), at.tp_of(at.y_peer(j), 1 - at.c))
        return remote(part.at[r, c], core_in.at[i, j], sc.at[i, j], rc.at[i, j], at.partner)

    def y_copy(i, j):
        return remote(
            y_out.at[i, j],
            y_in.at[i, j],
            sy.at[i, j],
            ry.at[i, j],
            (at.s, at.tp_of(at.y_peer(j), at.c)),
        )

    def home_copy(i):
        return remote(
            ret_out.at[i],
            ret_in.at[pl.ds(aligned(at.s, rows), rows), :],
            sr.at[i],
            rr.at[i],
            (peer_of(i), at.t),
        )

    at.barrier()

    def send_core(i, _):
        for j in range(at.ny):
            core_copy(i, j).start()
        return 0

    lax.fori_loop(0, n_sp, send_core, 0)

    def reduce_core(i):
        peer = peer_of(i)
        for j in list(range(1, at.ny)) + [0]:
            core_copy(i, j).wait_recv()
            r, c = piece(peer, at.tp_of(at.y_peer(j), at.c))
            both = part[r, c].astype(jnp.float32) + core_in[i, j].astype(jnp.float32)
            if j:
                y_out[i, j] = both.astype(jnp.bfloat16)
                y_copy(i, j).start()
            else:
                own_sum[i] = both

    def reduce_y(i):
        total = own_sum[i]
        for j in range(1, at.ny):
            y_copy(i, j).wait_recv()
            total = total + y_in[i, j].astype(jnp.float32)
        return total.astype(jnp.bfloat16)

    def send_home(i):
        ret_out[i] = reduce_y(i)
        home_copy(i).start()

    reduce_core(0)

    def step(i, _):
        reduce_core(i)
        send_home(i - 1)
        return 0

    lax.fori_loop(1, n_sp, step, 0)
    ret_in[pl.ds(aligned(at.s, rows), rows), :] = reduce_y(n_sp - 1)

    def wait_home(i, _):
        source = at.sp_source(i + 1)
        spot = ret_in.at[pl.ds(aligned(source, rows), rows), :]
        remote(ret_out.at[i], spot, sr.at[i], rr.at[i], (peer_of(i), at.t)).wait_recv()
        return 0

    lax.fori_loop(0, n_sp - 1, wait_home, 0)
    own_cols = cot[:, pl.ds(aligned(at.t, cols), cols)].astype(jnp.float32)
    pair_sum = jnp.dot(pick[...], ret_in[...], preferred_element_type=jnp.float32)
    low[...] = (own_cols + pair_sum).astype(jnp.bfloat16)

    def spot_of(tp):
        return out.at[:, pl.ds(aligned(tp, cols), cols)]

    def low_y(j):
        return remote(
            low, spot_of(at.t), sl.at[j], rl.at[j], (at.s, at.tp_of(at.y_peer(j), at.c))
        )

    def low_y_in(j):
        return remote(
            low,
            spot_of(at.tp_of(at.y_source(j), at.c)),
            sl.at[j],
            rl.at[j],
            (at.s, at.tp_of(at.y_peer(j), at.c)),
        )

    def low_core(j, outgoing):
        spot = spot_of(at.tp_of(at.y_source(j), at.c if outgoing else 1 - at.c))
        src = low if j == 0 else spot
        return remote(src, spot, sp_.at[j], rp_.at[j], at.partner)

    for j in range(1, at.ny):
        low_y(j).start()
    low_core(0, True).start()
    own = pltpu.make_async_copy(low, spot_of(at.t), own_sem)
    own.start()
    for j in range(1, at.ny):
        low_y_in(j).wait_recv()
        low_core(j, True).start()
    own.wait()
    for j in range(at.ny):
        low_core(j, False).wait_recv()
        low_core(j, True).wait_send()
    for j in range(1, at.ny):
        low_y(j).wait_send()

    def drain(i, _):
        for j in range(at.ny):
            core_copy(i, j).wait_send()
        for j in range(1, at.ny):
            y_copy(i, j).wait_send()
        return 0

    def drain_home(i, _):
        home_copy(i).wait_send()
        return 0

    lax.fori_loop(0, n_sp, drain, 0)
    lax.fori_loop(0, n_sp - 1, drain_home, 0)


def give_back(part, pick, cot, n_sp, n_tp):
    total, width = part.shape
    rows, cols, ny, tok = total // n_sp, width // n_tp, n_tp // CORES, cot.shape[0]
    dma = pltpu.SemaphoreType.DMA
    bf = jnp.bfloat16
    return pl.pallas_call(
        functools.partial(return_kernel, n_sp, n_tp),
        out_shape=jax.ShapeDtypeStruct((tok, width), bf),
        in_specs=[pl.BlockSpec(memory_space=pltpu.VMEM)] * 3,
        out_specs=pl.BlockSpec(memory_space=pltpu.VMEM),
        scratch_shapes=[
            pltpu.VMEM((n_sp, ny, rows, cols), bf),
            pltpu.VMEM((n_sp, rows, cols), jnp.float32),
            pltpu.VMEM((n_sp, ny, rows, cols), bf),
            pltpu.VMEM((n_sp, ny, rows, cols), bf),
            pltpu.VMEM((n_sp, rows, cols), bf),
            pltpu.VMEM((n_sp * rows, cols), bf),
            pltpu.VMEM((tok, cols), bf),
            dma((n_sp, ny)),
            dma((n_sp, ny)),
            dma((n_sp, ny)),
            dma((n_sp, ny)),
            dma((n_sp,)),
            dma((n_sp,)),
            dma((ny,)),
            dma((ny,)),
            dma((ny,)),
            dma((ny,)),
            dma,
        ],
        compiler_params=pltpu.CompilerParams(
            collective_id=1, has_side_effects=True, vmem_limit_bytes=VMEM_LIMIT
        ),
    )(part, pick, cot)


def close_kernel(n_sp, n_tp, part, link, proj, carry, held, links, sg, rg, sk, rk):
    at = Place(n_sp, n_tp)
    rows = part.shape[0] // n_sp

    def proj_copy(i):
        peer = at.sp_peer(i)
        return remote(
            part.at[pl.ds(aligned(peer, rows), rows), :],
            held.at[i],
            sg.at[i],
            rg.at[i],
            (peer, at.t),
        )

    def link_copy(i):
        return remote(link, links.at[i], sk.at[i], rk.at[i], (at.sp_peer(i), at.t))

    at.barrier(False)

    def send_link(i, _):
        link_copy(i).start()
        return 0

    def send_proj(i, _):
        proj_copy(i).start()
        return 0

    lax.fori_loop(1, n_sp, send_link, 0)
    lax.fori_loop(1, n_sp, send_proj, 0)

    def compose(k, state):
        i = k + 1
        link_copy(i).wait_recv()
        ahead = n_sp - i
        later = at.s + ahead < n_sp
        lower = links[i]
        return jnp.where(later, lower[0:1] * state + lower[1:2], state)

    carry[...] = lax.fori_loop(0, n_sp - 1, compose, jnp.zeros(carry.shape, jnp.float32))

    proj[...] = part[pl.ds(aligned(at.s, rows), rows), :].astype(jnp.float32)

    def add(i, _):
        proj_copy(i).wait_recv()
        proj[...] += held[i].astype(jnp.float32)
        return 0

    lax.fori_loop(1, n_sp, add, 0)

    def drain(i, _):
        link_copy(i).wait_send()
        proj_copy(i).wait_send()
        return 0

    lax.fori_loop(1, n_sp, drain, 0)


def close(part, link, n_sp, n_tp):
    total, channels = part.shape
    dma = pltpu.SemaphoreType.DMA
    return pl.pallas_call(
        functools.partial(close_kernel, n_sp, n_tp),
        out_shape=(
            jax.ShapeDtypeStruct((total // n_sp, channels), jnp.float32),
            jax.ShapeDtypeStruct((1, channels), jnp.float32),
        ),
        in_specs=[pl.BlockSpec(memory_space=pltpu.VMEM)] * 2,
        out_specs=[pl.BlockSpec(memory_space=pltpu.VMEM)] * 2,
        scratch_shapes=[
            pltpu.VMEM((n_sp, total // n_sp, channels), jnp.bfloat16),
            pltpu.VMEM((n_sp,) + link.shape, jnp.float32),
            dma((n_sp,)),
            dma((n_sp,)),
            dma((n_sp,)),
            dma((n_sp,)),
        ],
        compiler_params=pltpu.CompilerParams(
            collective_id=2, has_side_effects=True, vmem_limit_bytes=VMEM_LIMIT
        ),
    )(part, link)


def local(
    stream,
    cotangent,
    route_ids,
    route_weights,
    w_gate,
    w_up,
    w_down,
    out_proj,
    mixed,
    rec_input,
    branch_input,
    state_before,
    rec_gates,
    in_gates,
    decay_param,
    decay_shift,
):
    sp_count, tp_count = lax.axis_size("sp"), lax.axis_size("tp")
    tok_rows, model_width = cotangent.shape
    top_count = route_ids.shape[1]
    local_experts = w_gate.shape[0]
    expert_count = local_experts * sp_count
    capacity = 2 * tok_rows * top_count // expert_count
    slots = expert_count * capacity
    share_cols = model_width // tp_count
    flat_ids = route_ids.reshape(-1)
    pair_at = jnp.arange(flat_ids.shape[0], dtype=jnp.int32)
    earlier = (flat_ids[:, None] == flat_ids[None, :]) & (pair_at[None, :] < pair_at[:, None])
    slot_index = jnp.sum(earlier.astype(jnp.int32), axis=1)
    target = (flat_ids * capacity + slot_index).reshape(tok_rows, top_count)
    slot_at = jnp.arange(slots, dtype=jnp.int32)
    lands = [target[:, k][None, :] == slot_at[:, None] for k in range(top_count)]
    lands_any = functools.reduce(jnp.logical_or, lands)
    pick = functools.reduce(
        jnp.logical_or, [target[:, k][:, None] == slot_at[None, :] for k in range(top_count)]
    ).astype(jnp.bfloat16)
    first_col = lax.axis_index("tp") * share_cols
    own_stream = lax.dynamic_slice_in_dim(stream, first_col, share_cols, 1)
    own_cot = lax.dynamic_slice_in_dim(cotangent, first_col, share_cols, 1)
    scaled = [
        (route_weights[:, k : k + 1] * own_cot.astype(jnp.float32)).astype(jnp.bfloat16)
        for k in range(top_count)
    ]
    tok_src = jnp.dot(
        lands_any.astype(jnp.bfloat16), own_stream, preferred_element_type=jnp.float32
    ).astype(jnp.bfloat16)
    grd_src = jnp.dot(
        jnp.concatenate(lands, axis=1).astype(jnp.bfloat16),
        jnp.concatenate(scaled, axis=0),
        preferred_element_type=jnp.float32,
    ).astype(jnp.bfloat16)
    tokens_in, grads_in = dispatch(tok_src, grd_src, sp_count, tp_count)
    grads_in = grads_in.reshape(sp_count, local_experts, capacity, model_width)
    tokens_in = tokens_in.reshape(sp_count, local_experts, capacity, model_width)
    gate_pre = jnp.einsum("secd,edf->secf", tokens_in, w_gate, preferred_element_type=jnp.float32)
    up_pre = jnp.einsum("secd,edf->secf", tokens_in, w_up, preferred_element_type=jnp.float32)
    act_val, act_vjp = jax.vjp(expert_act, gate_pre, up_pre)
    act_low = act_val.astype(jnp.bfloat16)
    d_act = jnp.einsum("secd,efd->secf", grads_in, w_down, preferred_element_type=jnp.float32)
    d_gate, d_up = act_vjp(d_act)
    d_gate = d_gate.astype(jnp.bfloat16)
    d_up = d_up.astype(jnp.bfloat16)
    grad_gate, grad_up, grad_down = weight_grads(tokens_in, grads_in, d_gate, d_up, act_low)
    partial_value = jnp.einsum("secf,edf->secd", d_gate, w_gate, preferred_element_type=jnp.float32)
    partial_value = partial_value + jnp.einsum(
        "secf,edf->secd", d_up, w_up, preferred_element_type=jnp.float32
    )
    partial_low = partial_value.astype(jnp.bfloat16).reshape(slots, model_width)
    stream_low = give_back(partial_low, pick, cotangent, sp_count, tp_count)
    d_mixed = lax.dot_general(
        out_proj, stream_low, (((0,), (1,)), ((), ())), preferred_element_type=jnp.float32
    )
    proj_part = lax.dot_general(
        stream_low, mixed, (((0,), (1,)), ((), ())), preferred_element_type=jnp.float32
    ).astype(jnp.bfloat16)
    channels, positions = rec_input.shape
    gate_heads = rec_gates.shape[0]
    head_dim = rec_gates.shape[1]
    rec_heads = rec_input.reshape(gate_heads, head_dim, positions)
    rec_pre = jnp.einsum(
        "hij,hit->hjt", rec_gates, rec_heads, preferred_element_type=jnp.float32
    ).reshape(channels, positions)
    in_pre = jnp.einsum(
        "hij,hit->hjt", in_gates, rec_heads, preferred_element_type=jnp.float32
    ).reshape(channels, positions)
    rec_gate = jax.nn.sigmoid(rec_pre)
    in_gate = jax.nn.sigmoid(in_pre)
    soft_plus = jax.nn.softplus(-decay_param)[:, None]
    log_decay = -RATE_SCALE * rec_gate * soft_plus + decay_shift
    decay_rate = jnp.exp(log_decay)
    token_position = lax.axis_index("sp") * positions + jnp.arange(positions, dtype=jnp.int32)
    at_start = (token_position == 0)[None, :]
    raw_mult = jnp.sqrt(-jnp.expm1(2.0 * log_decay))
    multiplier = jnp.where(at_start, 1.0, raw_mult)
    rec_value = rec_input.astype(jnp.float32)
    state_now = decay_rate * state_before + multiplier * in_gate * rec_value
    gelu_val, gelu_vjp = jax.vjp(jax.nn.gelu, branch_input.astype(jnp.float32))
    grad_branch = gelu_vjp(d_mixed * state_now)[0]
    d_state = d_mixed * gelu_val
    next_decay = jnp.concatenate([decay_rate[:, 1:], jnp.zeros((channels, 1), jnp.float32)], axis=1)
    local_adj = lax.associative_scan(reverse_step, (next_decay, d_state), reverse=True, axis=1)[1]
    log_cumsum = jnp.cumsum(log_decay, axis=1)
    total_log = log_cumsum[:, -1:]
    tail_decay = jnp.exp(total_log - log_cumsum)
    device_prod = jnp.exp(total_log[:, 0])
    head_term = decay_rate[:, 0] * local_adj[:, 0]
    link = jnp.concatenate(
        [device_prod[None], head_term[None], jnp.zeros((6, channels), jnp.float32)], axis=0
    )
    grad_proj, carried = close(proj_part, link, sp_count, tp_count)
    adjoint = local_adj + tail_decay * carried[0][:, None]
    mult_term = adjoint * in_gate * rec_value * decay_rate * decay_rate / raw_mult
    d_log = adjoint * state_before * decay_rate - jnp.where(at_start, 0.0, mult_term)
    d_rec_pre = (d_log * -RATE_SCALE * soft_plus * rec_gate * (1.0 - rec_gate)).astype(jnp.bfloat16)
    d_in_pre = (adjoint * multiplier * rec_value * in_gate * (1.0 - in_gate)).astype(jnp.bfloat16)
    back_rec = jnp.einsum(
        "hij,hjt->hit",
        rec_gates,
        d_rec_pre.reshape(gate_heads, head_dim, positions),
        preferred_element_type=jnp.float32,
    )
    back_in = jnp.einsum(
        "hij,hjt->hit",
        in_gates,
        d_in_pre.reshape(gate_heads, head_dim, positions),
        preferred_element_type=jnp.float32,
    )
    grad_rec = adjoint * multiplier * in_gate + (back_rec + back_in).reshape(channels, positions)
    return (grad_gate, grad_up, grad_down, grad_proj, grad_rec, grad_branch)


def solution(mesh):
    placed = (
        P("sp", None),
        P("sp", None),
        P("sp", None),
        P("sp", None),
        P("sp", None, "tp"),
        P("sp", None, "tp"),
        P("sp", "tp", None),
        P(None, "tp"),
        P("tp", "sp"),
        P("tp", "sp"),
        P("tp", "sp"),
        P("tp", "sp"),
        P("tp", None, None),
        P("tp", None, None),
        P("tp"),
        P("tp", "sp"),
    )
    return jax.shard_map(
        local,
        mesh=mesh,
        in_specs=placed,
        out_specs=(
            P("sp", None, "tp"),
            P("sp", None, "tp"),
            P("sp", "tp", None),
            P("sp", "tp"),
            P("tp", "sp"),
            P("tp", "sp"),
        ),
        check_vma=False,
    )
```
